768 devices in a mesh: fs: 96 (over z, y), tp: 8 (over x, core).
Axes of the slice: x: 4, y: 8, z: 12, core: 2. Of those that a mesh axis runs over, the one named last changes fastest.
Arguments:
- stream_in: bfloat16 [24576, 2112], P('fs'), may hold values from -6 to 6
- norm_gains: float32 [6, 2112], replicated, may hold values from 0.1 to 1.9
- gate_proj: bfloat16 [2112, 3072], P('fs', 'tp'), may hold values from -0.125 to 0.125
- up_proj: bfloat16 [2112, 3072], P('fs', 'tp'), may hold values from -0.125 to 0.125
- down_proj: bfloat16 [2112, 3072], P('fs', 'tp'), may hold values from -0.109375 to 0.109375
- outer_gate: bfloat16 [2112, 1056], P('fs', 'tp'), may hold values from -0.125 to 0.125
- inner_gate: bfloat16 [2112, 1056], P('fs', 'tp'), may hold values from -0.125 to 0.125
- value_proj: bfloat16 [2112, 1056], P('fs', 'tp'), may hold values from -0.125 to 0.125
- mixer_out: bfloat16 [2112, 1056], P('fs', 'tp'), may hold values from -0.1875 to 0.1875
- conv_taps: bfloat16 [3, 1056], replicated, may hold values from -3 to 3
Outputs:
- stream_out: bfloat16 [24576, 2112], P('fs')
The draws below stay inside these ranges and needn't reach their ends.
All inputs are finite; a program needn't handle non-finite values.
Results may differ from the reference program's by a relative error of at most 0.02.
Values may be sent and summed in bfloat16 or wider, within the bound.
A program may use at most 64 MiB of HBM per device.

```python
import jax
import jax.numpy as jnp
from jax import lax

D = 2112
FF = 3072
CW = 1056
CONV_K = 3
ROWS = 256
TOKENS = 24576
N_FS = 96
N_TP = 8


def shard_levels(key, dims, split, low, high):
    factor_of, own = 1.0, jax.random.fold_in(key, 6)
    for position, parts in split:
        steps = jnp.exp(jax.random.uniform(jax.random.fold_in(own, position), (parts,), jnp.float32, low / len(split), high / len(split)))
        factor_of = factor_of * jnp.repeat(steps, dims[position] // parts).reshape([-1 if axis == position else 1 for axis in range(len(dims))])
    return factor_of


def bell_draw(own_key, dims, width, most, split=(), held_as=jnp.bfloat16):
    values = jax.random.normal(own_key, dims, jnp.float32) * width
    if len(split) > 0:
        values = shard_levels(own_key, dims, split, -0.22, 0.18) * values
    return jnp.clip(values, min=-most, max=most).astype(held_as)


def setup_inputs(seed: int = 0) -> dict:
    key_of = jax.random.split(jax.random.key(seed), 11)
    stream_in = bell_draw(key_of[0], (TOKENS, D), 1.0, 6.0, ((0, 96),))
    norm_gains = jnp.clip(1.0 + 0.18 * jax.random.normal(key_of[1], (6, D), jnp.float32), 0.1, 1.9)
    gate_proj = bell_draw(key_of[2], (D, FF), D ** -0.5, 0.125, ((0, 96), (1, 8)))
    up_proj = bell_draw(key_of[3], (D, FF), D ** -0.5, 0.125, ((0, 96), (1, 8)))
    down_proj = bell_draw(key_of[4], (D, FF), FF ** -0.5, 0.109375, ((0, 96), (1, 8)))
    outer_gate = bell_draw(key_of[5], (D, CW), D ** -0.5, 0.125, ((0, 96), (1, 8)))
    inner_gate = bell_draw(key_of[6], (D, CW), D ** -0.5, 0.125, ((0, 96), (1, 8)))
    value_proj = bell_draw(key_of[7], (D, CW), D ** -0.5, 0.125, ((0, 96), (1, 8)))
    mixer_out = bell_draw(key_of[8], (D, CW), CW ** -0.5, 0.1875, ((0, 96), (1, 8)))
    conv_taps = bell_draw(key_of[9], (CONV_K, CW), 0.577, 3.0)
    return dict(stream_in=stream_in, norm_gains=norm_gains, gate_proj=gate_proj, up_proj=up_proj, down_proj=down_proj, outer_gate=outer_gate, inner_gate=inner_gate, value_proj=value_proj, mixer_out=mixer_out, conv_taps=conv_taps)


EPSILON = 1e-06

def scaled(values, gain):
    return values * lax.rsqrt(lax.optimization_barrier(jnp.mean(values * values, axis=-1, keepdims=True)) + EPSILON) * gain

def block_sum(inner, weight):
    span_width = inner.shape[1] // N_TP
    total = jnp.zeros((inner.shape[0], weight.shape[0]), jnp.float32)
    for shard_index in range(N_TP):
        left = inner[:, shard_index * span_width:(shard_index + 1) * span_width]
        right = weight[:, shard_index * span_width:(shard_index + 1) * span_width]
        part = lax.dot_general(left, right, (((1,), (1,)), ((), ())), preferred_element_type=jnp.float32)
        total = total + lax.optimization_barrier(part.astype(jnp.bfloat16)).astype(jnp.float32)
    return total

def half_step(stream, norm_gains, first, gate_proj, up_proj, down_proj):
    normed = scaled(stream.astype(jnp.float32), norm_gains[first]).astype(jnp.bfloat16)
    gate = jnp.dot(normed, gate_proj, preferred_element_type=jnp.float32)
    upward = jnp.dot(normed, up_proj, preferred_element_type=jnp.float32)
    hidden = (jax.nn.silu(gate) * upward).astype(jnp.bfloat16)
    summed = block_sum(hidden, down_proj)
    result = stream.astype(jnp.float32) + 0.5 * scaled(summed, norm_gains[first + 1])
    return result.astype(jnp.bfloat16)

def reference(stream_in, norm_gains, gate_proj, up_proj, down_proj, outer_gate, inner_gate, value_proj, mixer_out, conv_taps):
    after_ffn = half_step(stream_in, norm_gains, 0, gate_proj, up_proj, down_proj)
    normed = scaled(after_ffn.astype(jnp.float32), norm_gains[2]).astype(jnp.bfloat16)
    outer = jnp.dot(normed, outer_gate, preferred_element_type=jnp.float32).astype(jnp.bfloat16)
    inner = jnp.dot(normed, inner_gate, preferred_element_type=jnp.float32).astype(jnp.bfloat16)
    value = jnp.dot(normed, value_proj, preferred_element_type=jnp.float32).astype(jnp.bfloat16)
    gated = (inner.astype(jnp.float32) * value.astype(jnp.float32)).reshape(N_FS, ROWS, CW)
    padded = jnp.pad(gated, ((0, 0), (CONV_K - 1, 0), (0, 0)))
    taps = conv_taps.astype(jnp.float32)
    conv = jnp.zeros_like(gated)
    for offset in range(CONV_K):
        conv = conv + taps[offset] * padded[:, offset:offset + ROWS]
    mixed = (outer.astype(jnp.float32) * conv.reshape(N_FS * ROWS, CW)).astype(jnp.bfloat16)
    summed = block_sum(mixed, mixer_out)
    after_mixer = (after_ffn.astype(jnp.float32) + scaled(summed, norm_gains[3])).astype(jnp.bfloat16)
    return half_step(after_mixer, norm_gains, 4, gate_proj, up_proj, down_proj)
```

```python
import jax
import jax.numpy as jnp
from jax import lax
from jax.experimental import pallas as pl
from jax.experimental.pallas import tpu as pltpu
from jax.sharding import PartitionSpec as P

EPSILON = 1e-06
NX, NY, NZ = 4, 8, 12
D = 2112
OWN = 22
PAD = 24
DP = 96 * PAD
QN, QW = 3, DP // 3
HALF, SHARE = 128, 32
HID, CH = 384, 132
CW_A, CW_B = 896, 896
F32, BF16 = jnp.float32, jnp.bfloat16


def windows():
    out = []
    for j in range(6):
        base = (352 * j) // 128 * 128
        out.append((j, base, min(512, D - base)))
    return out


def spread(j, base, width):
    row = lax.broadcasted_iota(jnp.int32, (width, 384), 0).astype(F32) + float(base)
    col = lax.broadcasted_iota(jnp.int32, (width, 384), 1).astype(F32)
    block = jnp.floor((col + 0.5) / float(PAD))
    inside = col - block * float(PAD)
    target = float(352 * j) + block * float(OWN) + inside
    hit = (row == target) & (inside < float(OWN) - 0.5)
    return jnp.where(hit, 1.0, 0.0).astype(BF16)


def dot(a, b):
    return lax.dot_general(a, b, (((1,), (0,)), ((), ())), preferred_element_type=F32)


def dot_t(a, b):
    return lax.dot_general(a, b, (((1,), (1,)), ((), ())), preferred_element_type=F32)


def kernel(
    wa_in, wb_in, stream, gains, taps, out,
    wa, wb, xs, xn, hid, part, got, tot, res, fin, acc, halo_out, halo_in,
    g_send, g_recv, p_send, p_recv, rs_send, rs_recv, ag_send, ag_recv,
    fo_send, fo_recv, fp_send, fp_recv, h_send, h_recv, l_sem,
):
    fs, tp = lax.axis_index("fs"), lax.axis_index("tp")
    z, y = fs // NY, fs % NY
    x, c = tp // 2, tp % 2
    s = 1 - 2 * c

    def at(zz, yy, xx, cc):
        return {"fs": zz * NY + yy, "tp": xx * 2 + cc}

    def ymod(v):
        return lax.rem(v + NY, NY)

    def zmod(v):
        return lax.rem(v + NZ, NZ)

    here = [wa.at[c, z, pl.ds(pl.multiple_of(y * PAD, 8), PAD), :], wb.at[c, z, pl.ds(pl.multiple_of(y * PAD, 8), PAD), :]]
    own = [pltpu.make_async_copy(src, dst, l_sem.at[i]) for i, (src, dst) in enumerate(zip((wa_in, wb_in), here))]
    for copy in own:
        copy.start()

    y_fwd, y_back = at(z, ymod(y + s), x, c), at(z, ymod(y - s), x, c)
    z_fwd, z_back = at(zmod(z + s), y, x, c), at(zmod(z - s), y, x, c)
    mate = at(z, y, x, 1 - c)
    peers = [at(z, y, lax.rem(x + d, NX), c) for d in (1, 2, 3)]
    barrier = pltpu.get_barrier_semaphore()
    for dev in [y_fwd, y_back, z_fwd, z_back, mate] + peers:
        pl.semaphore_signal(barrier, inc=1, device_id=dev, device_id_type=pl.DeviceIdType.MESH)
    pl.semaphore_wait(barrier, 8)
    for copy in own:
        copy.wait()

    ys = [y] + [ymod(y - s * d) for d in range(1, 5)] + [ymod(y + s * d) for d in range(1, 4)]
    zs = [z] + [zmod(z - s * d) for d in range(1, 7)] + [zmod(z + s * d) for d in range(1, 6)]
    bufs = (wa, wb)

    def remote(which, src_zz, src_yy, index, dev):
        ref = bufs[which].at[c, src_zz, pl.ds(pl.multiple_of(src_yy * PAD, 8), PAD), :]
        return pltpu.make_async_remote_copy(
            src_ref=ref, dst_ref=ref, send_sem=g_send.at[which, index], recv_sem=g_recv.at[which, index],
            device_id=dev, device_id_type=pl.DeviceIdType.MESH,
        )

    started = []

    def push(which, jz, jy, to_jz, to_jy, dev):
        copy = remote(which, zs[jz], ys[jy], to_jz * NY + to_jy, dev)
        copy.start()
        started.append(copy)

    def take(which, jz, jy):
        remote(which, zs[jz], ys[jy], jz * NY + jy, y_fwd).wait_recv()

    y_hops = ((0, 4, y_fwd), (4, 3, y_back))
    z_hops = ((0, 6, z_fwd), (6, 5, z_back))

    def y_next(which, jz, jy):
        for off, hops, dev in y_hops:
            if jy == 0:
                push(which, jz, 0, jz, off + 1, dev)
            elif off < jy < off + hops:
                push(which, jz, jy, jz, jy + 1, dev)

    def z_next(which, jz, jy):
        for off, hops, dev in z_hops:
            if jz == 0:
                push(which, 0, jy, off + 1, jy, dev)
            elif off < jz < off + hops:
                push(which, jz, jy, jz + 1, jy, dev)

    def y_far(jy):
        return jy if jy <= 4 else jy - 4

    def z_far(jz):
        return jz if jz <= 6 else jz - 6

    mates = []

    def to_mate(which, sub, index):
        ref = bufs[which].at[c, zs[index], pl.ds(0, NY * PAD), :] if which == 0 else sub
        copy = pltpu.make_async_remote_copy(
            src_ref=ref, dst_ref=ref, send_sem=p_send.at[which, index], recv_sem=p_recv.at[which, index],
            device_id=mate, device_id_type=pl.DeviceIdType.MESH,
        )
        copy.start()
        mates.append(copy)

    y_order = [0, 1, 5, 2, 6, 3, 7, 4]
    z_order = [0, 1, 7, 2, 8, 3, 9, 4, 10, 5, 11, 6]

    z_next(0, 0, 0)
    y_next(1, 0, 0)
    y_next(0, 0, 0)
    z_next(1, 0, 0)

    half = stream[pl.ds(pl.multiple_of(c * HALF, HALF), HALF), :]
    mine = stream[pl.ds(pl.multiple_of(c * HALF + x * SHARE, SHARE), SHARE), :]
    for j, base, width in windows():
        m = spread(j, base, width)
        xs[:, 384 * j:384 * (j + 1)] = dot(half[:, base:base + width], m).astype(BF16)
        res[:, 384 * j:384 * (j + 1)] = dot(mine[:, base:base + width], m).astype(BF16)
    wide = xs[...].astype(F32)
    scale = lax.rsqrt(jnp.sum(wide * wide, axis=-1, keepdims=True) / D + EPSILON)
    for q in range(QN):
        cols = slice(q * QW, (q + 1) * QW)
        xn[q] = (wide[:, cols] * scale * gains[0:1, cols]).astype(BF16)

    for slot in range(1, 11):
        for jy in y_order:
            if y_far(jy) == slot:
                take(0, 0, jy)
                z_next(0, 0, jy)
                y_next(0, 0, jy)
        for jz in z_order:
            if z_far(jz) == slot:
                take(1, jz, 0)
                y_next(1, jz, 0)
                z_next(1, jz, 0)
        for jz in z_order:
            for jy in y_order:
                if y_far(jy) + z_far(jz) == slot:
                    if jz > 0:
                        take(0, jz, jy)
                        z_next(0, jz, jy)
                    if jy > 0:
                        take(1, jz, jy)
                        y_next(1, jz, jy)
        for jz in range(NZ):
            if slot == 4 + z_far(jz):
                to_mate(0, None, jz)
        for jy in range(NY):
            if slot == 6 + y_far(jy):
                to_mate(1, wb.at[c, :, pl.ds(pl.multiple_of(ys[jy] * PAD, 8), PAD), :], jy)
    for copy in mates:
        copy.wait_recv()

    def weight(buf, w, q, lo, hi):
        return buf[w, 4 * q:4 * q + 4, 0:NY * PAD, lo:hi].reshape(QW, hi - lo)

    def project(buf, w, lo, hi):
        total = dot(xn[0], weight(buf, w, 0, lo, hi))
        for q in range(1, QN):
            total = total + dot(xn[q], weight(buf, w, q, lo, hi))
        return total

    def narrow(layer, parts, gain, factor, last):
        copies = []
        for q in range(QN):
            total = parts(q)
            part[layer, q] = total.astype(BF16)
            for d in (2, 1, 3):
                there = lax.rem(x + d, NX)
                copy = pltpu.make_async_remote_copy(
                    src_ref=part.at[layer, q, pl.ds(pl.multiple_of(there * SHARE, SHARE), SHARE), :],
                    dst_ref=got.at[d - 1, q],
                    send_sem=rs_send.at[layer, d - 1, q], recv_sem=rs_recv.at[layer, d - 1, q],
                    device_id=peers[d - 1], device_id_type=pl.DeviceIdType.MESH,
                )
                copy.start()
                copies.append((q, copy))
        squares = jnp.zeros((SHARE, 1), F32)
        for q in range(QN):
            for at_q, copy in copies:
                if at_q == q:
                    copy.wait_recv()
            total = part[layer, q, pl.ds(pl.multiple_of(x * SHARE, SHARE), SHARE), :].astype(F32)
            for d in range(3):
                total = total + got[d, q].astype(F32)
            tot[:, q * QW:(q + 1) * QW] = total
            squares = squares + jnp.sum(total * total, axis=-1, keepdims=True)
        scale = lax.rsqrt(squares / D + EPSILON)
        fresh = (res[...].astype(F32) + factor * (tot[...] * scale * gains[gain:gain + 1, :])).astype(BF16)
        res[...] = fresh
        for _, copy in copies:
            copy.wait_send()
        if last:
            return
        wide = fresh.astype(F32)
        scale = lax.rsqrt(jnp.sum(wide * wide, axis=-1, keepdims=True) / D + EPSILON)
        rows = pl.ds(pl.multiple_of(x * SHARE, SHARE), SHARE)
        copies = []
        for q in range(QN):
            cols = slice(q * QW, (q + 1) * QW)
            xn[q, rows, :] = (wide[:, cols] * scale * gains[gain + 1:gain + 2, cols]).astype(BF16)
            for d in (2, 1, 3):
                copy = pltpu.make_async_remote_copy(
                    src_ref=xn.at[q, rows, :], dst_ref=xn.at[q, rows, :],
                    send_sem=ag_send.at[layer, d - 1, q], recv_sem=ag_recv.at[layer, d - 1, q],
                    device_id=peers[d - 1], device_id_type=pl.DeviceIdType.MESH,
                )
                copy.start()
                copies.append(copy)
        for copy in copies:
            copy.wait()

    def ffn(layer, gain, last):
        for w in range(2):
            gate = project(wa, w, 0, HID)
            up = project(wb, w, 0, HID)
            hid[:, w * HID:(w + 1) * HID] = (gate / (1.0 + jnp.exp(-gate)) * up).astype(BF16)

        def parts(q):
            total = None
            for w in range(2):
                a = dot_t(hid[:, w * HID:w * HID + 128], weight(wa, w, q, HID, HID + 128))
                b = dot_t(hid[:, w * HID + 128:(w + 1) * HID], weight(wb, w, q, HID, HID + 256))
                total = a + b if total is None else total + a + b
            return total

        narrow(layer, parts, gain, 0.5, last)

    ffn(0, 1, False)

    gated, outer = [], []
    for w in range(2):
        low = project(wa, w, 512, 896)
        high = project(wb, w, 640, 896)
        both = jnp.concatenate([low, high], axis=1).astype(BF16).astype(F32)
        outer.append(both[:, 0:CH])
        product = both[:, CH:2 * CH] * both[:, 2 * CH:3 * CH]
        gated.append(product)
        halo_out[w, :, 0:CH] = product[HALF - 8:HALF, :]
    hcopy = pltpu.make_async_remote_copy(
        src_ref=halo_out, dst_ref=halo_in, send_sem=h_send, recv_sem=h_recv,
        device_id=mate, device_id_type=pl.DeviceIdType.MESH,
    )
    hcopy.start()
    hcopy.wait()
    row = lax.broadcasted_iota(jnp.int32, (HALF, CH), 0)
    for w in range(2):
        before = jnp.where(c == 1, halo_in[w, :, 0:CH], 0.0)
        one, two = before[7:8, :], before[6:7, :]
        g = gated[w]
        back1 = jnp.where(row == 0, one, pltpu.roll(g, 1, 0))
        back2 = pltpu.roll(g, 2, 0)
        back2 = jnp.where(row == 0, two, jnp.where(row == 1, one, back2))
        conv = taps[w, 0:1, 0:CH] * back2 + taps[w, 1:2, 0:CH] * back1 + taps[w, 2:3, 0:CH] * g
        mixed = outer[w] * conv
        hid[:, w * 256:(w + 1) * 256] = jnp.concatenate(
            [jnp.zeros((HALF, 12), F32), mixed, jnp.zeros((HALF, 112), F32)], axis=1
        ).astype(BF16)

    def mixer_parts(q):
        return dot_t(hid[:, 0:256], weight(wb, 0, q, 640, 896)) + dot_t(hid[:, 256:512], weight(wb, 1, q, 640, 896))

    narrow(1, mixer_parts, 3, 1.0, False)
    ffn(2, 5, True)

    acc[...] = jnp.zeros_like(acc)
    for j, base, width in windows():
        m = spread(j, base, width)
        acc[:, base:base + width] += dot_t(res[:, 384 * j:384 * (j + 1)], m)
    rows = pl.ds(pl.multiple_of(c * HALF + x * SHARE, SHARE), SHARE)
    fin[rows, :] = acc[:, 0:D].astype(BF16)
    outs = []

    def result(index, rows, dev, sems):
        return pltpu.make_async_remote_copy(
            src_ref=fin.at[rows, :], dst_ref=fin.at[rows, :], send_sem=sems[0].at[index], recv_sem=sems[1].at[index],
            device_id=dev, device_id_type=pl.DeviceIdType.MESH,
        )

    for d in (2, 1, 3):
        copy = result(d, rows, peers[d - 1], (fo_send, fo_recv))
        copy.start()
        outs.append(copy)
    copy = result(0, rows, mate, (fp_send, fp_recv))
    copy.start()
    mate_outs = [copy]
    for d in (1, 3, 2):
        theirs = pl.ds(pl.multiple_of(c * HALF + lax.rem(x + NX - d, NX) * SHARE, SHARE), SHARE)
        result(d, theirs, mate, (fo_send, fo_recv)).wait_recv()
        copy = result(d, theirs, mate, (fp_send, fp_recv))
        copy.start()
        mate_outs.append(copy)
    for copy in mate_outs:
        copy.wait_recv()
    back = pltpu.make_async_copy(fin, out, l_sem.at[0])
    back.start()
    for copy in started + mates + outs + mate_outs:
        copy.wait_send()
    back.wait()


def local(stream_in, norm_gains, gate_proj, up_proj, down_proj, outer_gate, inner_gate, value_proj, mixer_out, conv_taps):
    mix = jnp.concatenate([outer_gate, inner_gate, value_proj, mixer_out], axis=1)
    mix = jnp.pad(mix, ((0, 0), (0, 640 - 4 * CH)))
    rows = ((0, PAD - OWN), (0, 0))
    wa_in = jnp.pad(jnp.concatenate([gate_proj, down_proj[:, :128], mix[:, :384]], axis=1), rows)
    wb_in = jnp.pad(jnp.concatenate([up_proj, down_proj[:, 128:], mix[:, 384:]], axis=1), rows)
    gains = jnp.pad(norm_gains.reshape(6, 96, OWN), ((0, 2), (0, 0), (0, PAD - OWN))).reshape(8, DP)
    x = lax.axis_index("tp") // 2
    taps = lax.dynamic_slice_in_dim(conv_taps, x * 2 * CH, 2 * CH, 1).astype(F32)
    taps = jnp.pad(jnp.moveaxis(taps.reshape(3, 2, CH), 1, 0), ((0, 0), (0, 5), (0, 256 - CH)))
    vmem = pl.BlockSpec(memory_space=pltpu.VMEM)
    hbm = pl.BlockSpec(memory_space=pl.ANY)
    dma = pltpu.SemaphoreType.DMA
    return pl.pallas_call(
        kernel,
        out_shape=jax.ShapeDtypeStruct((2 * HALF, D), BF16),
        in_specs=[hbm, hbm, vmem, vmem, vmem],
        out_specs=hbm,
        scratch_shapes=[
            pltpu.VMEM((2, NZ, NY * PAD + 8, CW_A), BF16),
            pltpu.VMEM((2, NZ, NY * PAD + 8, CW_B), BF16),
            pltpu.VMEM((HALF, DP), BF16),
            pltpu.VMEM((QN, HALF, QW), BF16),
            pltpu.VMEM((HALF, 2 * HID), BF16),
            pltpu.VMEM((3, QN, HALF, QW), BF16),
            pltpu.VMEM((3, QN, SHARE, QW), BF16),
            pltpu.VMEM((SHARE, DP), F32),
            pltpu.VMEM((SHARE, DP), BF16),
            pltpu.VMEM((2 * HALF, D), BF16),
            pltpu.VMEM((SHARE, 2176), F32),
            pltpu.VMEM((2, 8, 256), F32),
            pltpu.VMEM((2, 8, 256), F32),
            dma((2, 96)), dma((2, 96)),
            dma((2, 12)), dma((2, 12)),
            dma((3, 3, 3)), dma((3, 3, 3)),
            dma((2, 3, 3)), dma((2, 3, 3)),
            dma((4,)), dma((4,)),
            dma((4,)), dma((4,)),
            dma(()), dma(()),
            dma((2,)),
        ],
        compiler_params=pltpu.CompilerParams(
            collective_id=0, has_side_effects=True, vmem_limit_bytes=58 * 1024 * 1024
        ),
        name="layer",
    )(wa_in, wb_in, stream_in, gains, taps)


def solution(mesh):
    return jax.shard_map(
        local,
        mesh=mesh,
        in_specs=(
            P("fs", None), P(), P("fs", "tp"), P("fs", "tp"), P("fs", "tp"),
            P("fs", "tp"), P("fs", "tp"), P("fs", "tp"), P("fs", "tp"), P(),
        ),
        out_specs=P("fs", None),
        check_vma=False,
    )
```

```python
import jax
import jax.numpy as jnp
from jax import lax
from jax.experimental import pallas as pl
from jax.experimental.pallas import tpu as pltpu
from jax.sharding import PartitionSpec as P

EPSILON = 1e-06
NX, NY, NZ = 4, 8, 12
D = 2112
OWN = 22
PAD = 24
DP = 96 * PAD
QN, QW = 3, DP // 3
HALF, SHARE = 128, 32
HID, CH = 384, 132
LAG = 5
F32, BF16 = jnp.float32, jnp.bfloat16


def windows():
    out = []
    for j in range(6):
        base = (352 * j) // 128 * 128
        out.append((j, base, min(512, D - base)))
    return out


def spread(j, base, width):
    row = lax.broadcasted_iota(jnp.int32, (width, 384), 0).astype(F32) + float(base)
    col = lax.broadcasted_iota(jnp.int32, (width, 384), 1).astype(F32)
    block = jnp.floor((col + 0.5) / float(PAD))
    inside = col - block * float(PAD)
    target = float(352 * j) + block * float(OWN) + inside
    hit = (row == target) & (inside < float(OWN) - 0.5)
    return jnp.where(hit, 1.0, 0.0).astype(BF16)


def dot(a, b):
    return lax.dot_general(a, b, (((1,), (0,)), ((), ())), preferred_element_type=F32)


def dot_t(a, b):
    return lax.dot_general(a, b, (((1,), (1,)), ((), ())), preferred_element_type=F32)


def kernel(
    gate_in, up_in, down_in, outer_in, inner_in, value_in, mixer_in, stream_in, gains_in, taps_in, out,
    gate_sh, up_sh, down_sh, outer_sh, inner_sh, value_sh, mixer_sh, stream, gains_raw, taps_raw,
    wa, wb, ma, mb, xs, xn, proj, hid, part, got, tot, res, fin, acc, fout, gains, taps, halo_out, halo_in,
    g_send, g_recv, p_send, p_recv, rs_send, rs_recv, ag_send, ag_recv,
    fo_send, fo_recv, fp_send, fp_recv, h_send, h_recv, l_sem,
):
    fs, tp = lax.axis_index("fs"), lax.axis_index("tp")
    z, y = fs // NY, fs % NY
    x, c = tp // 2, tp % 2
    s = 1 - 2 * c

    def at(zz, yy, xx, cc):
        return {"fs": zz * NY + yy, "tp": xx * 2 + cc}

    def ymod(v):
        return lax.rem(v + NY, NY)

    def zmod(v):
        return lax.rem(v + NZ, NZ)

    arrivals = [
        pltpu.make_async_copy(src, dst, l_sem.at[i])
        for i, (src, dst) in enumerate((
            (gate_in, gate_sh), (up_in, up_sh), (down_in, down_sh), (outer_in, outer_sh), (inner_in, inner_sh),
            (value_in, value_sh), (mixer_in, mixer_sh), (stream_in, stream), (gains_in, gains_raw), (taps_in, taps_raw),
        ))
    ]
    for copy in arrivals:
        copy.start()

    y_fwd, y_back = at(z, ymod(y + s), x, c), at(z, ymod(y - s), x, c)
    z_fwd, z_back = at(zmod(z + s), y, x, c), at(zmod(z - s), y, x, c)
    mate = at(z, y, x, 1 - c)
    peers = [at(z, y, lax.rem(x + d, NX), c) for d in (1, 2, 3)]
    barrier = pltpu.get_barrier_semaphore()
    for dev in [y_fwd, y_back, z_fwd, z_back, mate] + peers:
        pl.semaphore_signal(barrier, inc=1, device_id=dev, device_id_type=pl.DeviceIdType.MESH)
    for copy in arrivals[:7]:
        copy.wait()

    def rows24(ref):
        return jnp.concatenate([ref[...].astype(F32), jnp.zeros((PAD - OWN, ref.shape[1]), F32)], axis=0)

    here = pl.ds(pl.multiple_of(y * PAD, 8), PAD)
    wa[c, z, here, 0:HID] = rows24(gate_sh).astype(BF16)
    wb[c, z, here, 0:HID] = rows24(up_sh).astype(BF16)
    down = rows24(down_sh).astype(BF16)
    wa[c, z, here, HID:HID + 128] = down[:, 0:128]
    wb[c, z, here, HID:HID + 256] = down[:, 128:HID]
    mix = jnp.concatenate(
        [rows24(outer_sh), rows24(inner_sh), rows24(value_sh), rows24(mixer_sh), jnp.zeros((PAD, 640 - 4 * CH), F32)], axis=1
    ).astype(BF16)
    ma[c, z, here, :] = mix[:, 0:384]
    mb[c, z, here, :] = mix[:, 384:640]
    pl.semaphore_wait(barrier, 8)

    ys = [y] + [ymod(y - s * d) for d in range(1, 5)] + [ymod(y + s * d) for d in range(1, 4)]
    zs = [z] + [zmod(z - s * d) for d in range(1, 7)] + [zmod(z + s * d) for d in range(1, 6)]
    bufs = (wa, wb, ma, mb)

    def remote(which, src_zz, src_yy, index, dev):
        ref = bufs[which].at[c, src_zz, pl.ds(pl.multiple_of(src_yy * PAD, 8), PAD), :]
        return pltpu.make_async_remote_copy(
            src_ref=ref, dst_ref=ref, send_sem=g_send.at[which, index], recv_sem=g_recv.at[which, index],
            device_id=dev, device_id_type=pl.DeviceIdType.MESH,
        )

    started = []

    def push(which, jz, jy, to_jz, to_jy, dev):
        copy = remote(which, zs[jz], ys[jy], to_jz * NY + to_jy, dev)
        copy.start()
        started.append(copy)

    def take(which, jz, jy):
        remote(which, zs[jz], ys[jy], jz * NY + jy, y_fwd).wait_recv()

    y_hops = ((0, 4, y_fwd), (4, 3, y_back))
    z_hops = ((0, 6, z_fwd), (6, 5, z_back))

    def y_next(which, jz, jy):
        for off, hops, dev in y_hops:
            if jy == 0:
                push(which, jz, 0, jz, off + 1, dev)
            elif off < jy < off + hops:
                push(which, jz, jy, jz, jy + 1, dev)

    def z_next(which, jz, jy):
        for off, hops, dev in z_hops:
            if jz == 0:
                push(which, 0, jy, off + 1, jy, dev)
            elif off < jz < off + hops:
                push(which, jz, jy, jz + 1, jy, dev)

    def y_far(jy):
        return jy if jy <= 4 else jy - 4

    def z_far(jz):
        return jz if jz <= 6 else jz - 6

    mates = []

    def to_mate(which, sub, index):
        ref = bufs[which].at[c, zs[index], pl.ds(0, NY * PAD), :] if which % 2 == 0 else sub
        copy = pltpu.make_async_remote_copy(
            src_ref=ref, dst_ref=ref, send_sem=p_send.at[which, index], recv_sem=p_recv.at[which, index],
            device_id=mate, device_id_type=pl.DeviceIdType.MESH,
        )
        copy.start()
        mates.append((which, copy))

    y_order = [0, 1, 5, 2, 6, 3, 7, 4]
    z_order = [0, 1, 7, 2, 8, 3, 9, 4, 10, 5, 11, 6]

    def own_out(group):
        even, odd = 2 * group, 2 * group + 1
        z_next(even, 0, 0)
        y_next(odd, 0, 0)
        y_next(even, 0, 0)
        z_next(odd, 0, 0)

    def slot_of(group, slot):
        even, odd = 2 * group, 2 * group + 1
        for jy in y_order:
            if y_far(jy) == slot:
                take(even, 0, jy)
                z_next(even, 0, jy)
                y_next(even, 0, jy)
        for jz in z_order:
            if z_far(jz) == slot:
                take(odd, jz, 0)
                y_next(odd, jz, 0)
                z_next(odd, jz, 0)
        for jz in z_order:
            for jy in y_order:
                if y_far(jy) + z_far(jz) == slot:
                    if jz > 0:
                        take(even, jz, jy)
                        z_next(even, jz, jy)
                    if jy > 0:
                        take(odd, jz, jy)
                        y_next(odd, jz, jy)
        for jz in range(NZ):
            if slot == 4 + z_far(jz):
                to_mate(even, None, jz)
        for jy in range(NY):
            if slot == 6 + y_far(jy):
                to_mate(odd, bufs[odd].at[c, :, pl.ds(pl.multiple_of(ys[jy] * PAD, 8), PAD), :], jy)

    def complete(group):
        for which, copy in mates:
            if which // 2 == group:
                copy.wait_recv()

    def window(j, base, width):
        m = spread(j, base, width)
        to = slice(384 * j, 384 * (j + 1))
        half = stream[base:base + width, pl.ds(pl.multiple_of(c * HALF, HALF), HALF)]
        xs[:, to] = lax.dot_general(half, m, (((0,), (0,)), ((), ())), preferred_element_type=F32).astype(BF16)
        res[:, to] = xs[pl.ds(pl.multiple_of(x * SHARE, SHARE), SHARE), to]
        left = gains_raw[:, base:base + width]
        total = None
        for _ in range(3):
            term = left.astype(BF16)
            left = left - term.astype(F32)
            moved = dot(term, m)
            total = moved if total is None else total + moved
        gains[0:6, to] = total

    def first_norm():
        wide = xs[...].astype(F32)
        scale = lax.rsqrt(jnp.sum(wide * wide, axis=-1, keepdims=True) / D + EPSILON)
        for q in range(QN):
            cols = slice(q * QW, (q + 1) * QW)
            xn[q] = (wide[:, cols] * scale * gains[0:1, cols]).astype(BF16)

    def own_taps():
        for w in range(2):
            row = lax.broadcasted_iota(jnp.int32, (8 * CH, 256), 0)
            col = lax.broadcasted_iota(jnp.int32, (8 * CH, 256), 1)
            pick = jnp.where((row == col + (2 * x + w) * CH) & (col < CH), 1.0, 0.0).astype(BF16)
            taps[w, 0:3, :] = dot(taps_raw[...], pick)

    own_out(0)
    for copy in arrivals[7:]:
        copy.wait()
    for slot in range(1, 11):
        slot_of(0, slot)
        if slot > LAG:
            slot_of(1, slot - LAG)
        if slot == LAG:
            own_out(1)
        if slot <= 6:
            window(*windows()[slot - 1])
        if slot == 7:
            first_norm()
        if slot == 8:
            own_taps()
    later = list(range(11 - LAG, 11))
    complete(0)

    def weight(buf, w, q, lo, hi):
        return buf[w, 4 * q:4 * q + 4, 0:NY * PAD, lo:hi].reshape(QW, hi - lo)

    def project(terms, incoming):
        for q in range(QN):
            for at_q, copy in incoming:
                if at_q == q:
                    copy.wait()
            for i, (buf, w, lo, hi) in enumerate(terms):
                value = dot(xn[q], weight(buf, w, q, lo, hi))
                if q == 0:
                    proj[i, :, 0:hi - lo] = value
                else:
                    proj[i, :, 0:hi - lo] += value

    def narrow(layer, parts, gain, factor, last, between=(), after=()):
        copies = []
        for q in range(QN):
            total = parts(q)
            part[layer, q] = total.astype(BF16)
            for d in (2, 1, 3):
                there = lax.rem(x + d, NX)
                copy = pltpu.make_async_remote_copy(
                    src_ref=part.at[layer, q, pl.ds(pl.multiple_of(there * SHARE, SHARE), SHARE), :],
                    dst_ref=got.at[d - 1, q],
                    send_sem=rs_send.at[layer, d - 1, q], recv_sem=rs_recv.at[layer, d - 1, q],
                    device_id=peers[d - 1], device_id_type=pl.DeviceIdType.MESH,
                )
                copy.start()
                copies.append((q, copy))
        for slot in between:
            slot_of(1, slot)
        squares = jnp.zeros((SHARE, 1), F32)
        for q in range(QN):
            for at_q, copy in copies:
                if at_q == q:
                    copy.wait_recv()
            total = part[layer, q, pl.ds(pl.multiple_of(x * SHARE, SHARE), SHARE), :].astype(F32)
            for d in range(3):
                total = total + got[d, q].astype(F32)
            tot[:, q * QW:(q + 1) * QW] = total
            squares = squares + jnp.sum(total * total, axis=-1, keepdims=True)
        scale = lax.rsqrt(squares / D + EPSILON)
        fresh = (res[...].astype(F32) + factor * (tot[...] * scale * gains[gain:gain + 1, :])).astype(BF16)
        res[...] = fresh
        for _, copy in copies:
            copy.wait_send()
        if last:
            return []
        wide = fresh.astype(F32)
        scale = lax.rsqrt(jnp.sum(wide * wide, axis=-1, keepdims=True) / D + EPSILON)
        rows = pl.ds(pl.multiple_of(x * SHARE, SHARE), SHARE)
        copies = []
        for q in range(QN):
            cols = slice(q * QW, (q + 1) * QW)
            xn[q, rows, :] = (wide[:, cols] * scale * gains[gain + 1:gain + 2, cols]).astype(BF16)
            for d in (2, 1, 3):
                copy = pltpu.make_async_remote_copy(
                    src_ref=xn.at[q, rows, :], dst_ref=xn.at[q, rows, :],
                    send_sem=ag_send.at[layer, d - 1, q], recv_sem=ag_recv.at[layer, d - 1, q],
                    device_id=peers[d - 1], device_id_type=pl.DeviceIdType.MESH,
                )
                copy.start()
                copies.append((q, copy))
        for slot in after:
            slot_of(1, slot)
        return copies

    def ffn(layer, gain, last, incoming, first=(), between=(), after=()):
        project(((wa, 0, 0, HID), (wb, 0, 0, HID), (wa, 1, 0, HID), (wb, 1, 0, HID)), incoming)
        for slot in first:
            slot_of(1, slot)
        for w in range(2):
            gate, up = proj[2 * w], proj[2 * w + 1]
            hid[:, w * HID:(w + 1) * HID] = (gate / (1.0 + jnp.exp(-gate)) * up).astype(BF16)

        def parts(q):
            total = None
            for w in range(2):
                a = dot_t(hid[:, w * HID:w * HID + 128], weight(wa, w, q, HID, HID + 128))
                b = dot_t(hid[:, w * HID + 128:(w + 1) * HID], weight(wb, w, q, HID, HID + 256))
                total = a + b if total is None else total + a + b
            return total

        return narrow(layer, parts, gain, 0.5, last, between, after)

    incoming = ffn(0, 1, False, [], later[:1], later[1:3], later[3:])
    complete(1)

    gated, outer = [], []
    project(((ma, 0, 0, 384), (mb, 0, 0, 256), (ma, 1, 0, 384), (mb, 1, 0, 256)), incoming)
    for w in range(2):
        both = jnp.concatenate([proj[2 * w], proj[2 * w + 1, :, 0:256]], axis=1).astype(BF16).astype(F32)
        outer.append(both[:, 0:CH])
        product = both[:, CH:2 * CH] * both[:, 2 * CH:3 * CH]
        gated.append(product)
        halo_out[w, :, 0:CH] = product[HALF - 8:HALF, :]
    hcopy = pltpu.make_async_remote_copy(
        src_ref=halo_out, dst_ref=halo_in, send_sem=h_send, recv_sem=h_recv,
        device_id=mate, device_id_type=pl.DeviceIdType.MESH,
    )
    hcopy.start()
    hcopy.wait()
    row = lax.broadcasted_iota(jnp.int32, (HALF, CH), 0)
    for w in range(2):
        before = jnp.where(c == 1, halo_in[w, :, 0:CH], 0.0)
        one, two = before[7:8, :], before[6:7, :]
        g = gated[w]
        back1 = jnp.where(row == 0, one, pltpu.roll(g, 1, 0))
        back2 = pltpu.roll(g, 2, 0)
        back2 = jnp.where(row == 0, two, jnp.where(row == 1, one, back2))
        conv = taps[w, 0:1, 0:CH] * back2 + taps[w, 1:2, 0:CH] * back1 + taps[w, 2:3, 0:CH] * g
        mixed = outer[w] * conv
        hid[:, w * 256:(w + 1) * 256] = jnp.concatenate(
            [jnp.zeros((HALF, 12), F32), mixed, jnp.zeros((HALF, 112), F32)], axis=1
        ).astype(BF16)

    def mixer_parts(q):
        return dot_t(hid[:, 0:256], weight(mb, 0, q, 0, 256)) + dot_t(hid[:, 256:512], weight(mb, 1, q, 0, 256))

    incoming = narrow(1, mixer_parts, 3, 1.0, False)
    ffn(2, 5, True, incoming)

    def mine_of(half, d):
        return pl.ds(pl.multiple_of(half * HALF + lax.rem(x + NX - d, NX) * SHARE, SHARE), SHARE)

    def result(index, rows, dev, sems):
        return pltpu.make_async_remote_copy(
            src_ref=fin.at[rows, :], dst_ref=fin.at[rows, :], send_sem=sems[0].at[index], recv_sem=sems[1].at[index],
            device_id=dev, device_id_type=pl.DeviceIdType.MESH,
        )

    fin[mine_of(c, 0), :] = res[...]
    outs, mate_outs = [], []
    for d in (2, 1, 3):
        outs.append(result(d, mine_of(c, 0), peers[d - 1], (fo_send, fo_recv)))
        outs[-1].start()
    for d in (0, 1, 3, 2):
        if d > 0:
            result(d, mine_of(c, d), mate, (fo_send, fo_recv)).wait_recv()
        mate_outs.append(result(d, mine_of(c, d), mate, (fp_send, fp_recv)))
        mate_outs[-1].start()
    backs = []
    for turn, h in enumerate((c, 1 - c)):
        if turn == 1:
            for copy in mate_outs:
                copy.wait_recv()
        tokens = pl.ds(pl.multiple_of(h * HALF, HALF), HALF)
        acc[...] = jnp.zeros_like(acc)
        for j, base, width in windows():
            acc[base:base + width, :] += dot_t(spread(j, base, width), fin[tokens, 384 * j:384 * (j + 1)])
        fout[turn] = acc[...].astype(BF16)
        backs.append(pltpu.make_async_copy(fout.at[turn], out.at[:, tokens], l_sem.at[turn]))
        backs[-1].start()
    for copy in started + [copy for _, copy in mates] + outs + mate_outs:
        copy.wait_send()
    for copy in backs:
        copy.wait()


def local(stream_in, norm_gains, gate_proj, up_proj, down_proj, outer_gate, inner_gate, value_proj, mixer_out, conv_taps):
    hbm = pl.BlockSpec(memory_space=pl.ANY)
    dma = pltpu.SemaphoreType.DMA
    return pl.pallas_call(
        kernel,
        out_shape=jax.ShapeDtypeStruct((D, 2 * HALF), BF16),
        in_specs=[hbm] * 10,
        out_specs=hbm,
        scratch_shapes=[
            pltpu.VMEM((OWN, HID), BF16), pltpu.VMEM((OWN, HID), BF16), pltpu.VMEM((OWN, HID), BF16),
            pltpu.VMEM((OWN, CH), BF16), pltpu.VMEM((OWN, CH), BF16), pltpu.VMEM((OWN, CH), BF16), pltpu.VMEM((OWN, CH), BF16),
            pltpu.VMEM((D, 2 * HALF), BF16), pltpu.VMEM((6, D), F32), pltpu.VMEM((3, 8 * CH), BF16),
            pltpu.VMEM((2, NZ, NY * PAD + 8, 512), BF16),
            pltpu.VMEM((2, NZ, NY * PAD + 8, 640), BF16),
            pltpu.VMEM((2, NZ, NY * PAD + 8, 384), BF16),
            pltpu.VMEM((2, NZ, NY * PAD + 8, 256), BF16),
            pltpu.VMEM((HALF, DP), BF16),
            pltpu.VMEM((QN, HALF, QW), BF16),
            pltpu.VMEM((4, HALF, HID), F32),
            pltpu.VMEM((HALF, 2 * HID), BF16),
            pltpu.VMEM((3, QN, HALF, QW), BF16),
            pltpu.VMEM((3, QN, SHARE, QW), BF16),
            pltpu.VMEM((SHARE, DP), F32),
            pltpu.VMEM((SHARE, DP), BF16),
            pltpu.VMEM((2 * HALF, DP), BF16),
            pltpu.VMEM((D, HALF), F32),
            pltpu.VMEM((2, D, HALF), BF16),
            pltpu.VMEM((8, DP), F32),
            pltpu.VMEM((2, 8, 256), F32),
            pltpu.VMEM((2, 8, 256), F32),
            pltpu.VMEM((2, 8, 256), F32),
            dma((4, 96)), dma((4, 96)),
            dma((4, 12)), dma((4, 12)),
            dma((3, 3, 3)), dma((3, 3, 3)),
            dma((2, 3, 3)), dma((2, 3, 3)),
            dma((4,)), dma((4,)),
            dma((4,)), dma((4,)),
            dma(()), dma(()),
            dma((10,)),
        ],
        compiler_params=pltpu.CompilerParams(
            collective_id=0, has_side_effects=True, vmem_limit_bytes=58 * 1024 * 1024
        ),
        name="layer",
    )(gate_proj, up_proj, down_proj, outer_gate, inner_gate, value_proj, mixer_out, stream_in.T, norm_gains, conv_taps).T


def solution(mesh):
    return jax.shard_map(
        local,
        mesh=mesh,
        in_specs=(
            P("fs", None), P(), P("fs", "tp"), P("fs", "tp"), P("fs", "tp"),
            P("fs", "tp"), P("fs", "tp"), P("fs", "tp"), P("fs", "tp"), P(),
        ),
        out_specs=P("fs", None),
        check_vma=False,
    )
```

```python
import jax
import jax.numpy as jnp
from jax import lax
from jax.experimental import pallas as pl
from jax.experimental.pallas import tpu as pltpu
from jax.sharding import PartitionSpec as P

EPSILON = 1e-06
NX, NY, NZ = 4, 8, 12
D = 2112
OWN = 22
PAD = 24
DP = 96 * PAD
QN, QW = 3, DP // 3
GROUPS, HALF = 2, 128
ROWS, SHARE = HALF // GROUPS, 16
HID, CH = 384, 132
LAG = 5
F32, BF16 = jnp.float32, jnp.bfloat16


def windows():
    out = []
    for j in range(6):
        base = (352 * j) // 128 * 128
        out.append((j, base, min(512, D - base)))
    return out


def spread(j, base, width):
    row = lax.broadcasted_iota(jnp.int32, (width, 384), 0).astype(F32) + float(base)
    col = lax.broadcasted_iota(jnp.int32, (width, 384), 1).astype(F32)
    block = jnp.floor((col + 0.5) / float(PAD))
    inside = col - block * float(PAD)
    target = float(352 * j) + block * float(OWN) + inside
    hit = (row == target) & (inside < float(OWN) - 0.5)
    return jnp.where(hit, 1.0, 0.0).astype(BF16)


def dot(a, b):
    return lax.dot_general(a, b, (((1,), (0,)), ((), ())), preferred_element_type=F32)


def dot_t(a, b):
    return lax.dot_general(a, b, (((1,), (1,)), ((), ())), preferred_element_type=F32)


def kernel(
    gate_in, up_in, down_in, outer_in, inner_in, value_in, mixer_in, stream_in, gains_in, taps_in, out,
    gate_sh, up_sh, down_sh, outer_sh, inner_sh, value_sh, mixer_sh, stream, gains_raw, taps_raw,
    wa, wb, ma, mb, xs, xn, proj, hid, part, got, tot, res, fin, acc, fout, gains, taps, halo_out, halo_in,
    g_send, g_recv, p_send, p_recv, rs_send, rs_recv, ag_send, ag_recv,
    fo_send, fo_recv, fp_send, fp_recv, h_send, h_recv, l_sem,
):
    fs, tp = lax.axis_index("fs"), lax.axis_index("tp")
    z, y = fs // NY, fs % NY
    x, c = tp // 2, tp % 2
    s = 1 - 2 * c

    def at(zz, yy, xx, cc):
        return {"fs": zz * NY + yy, "tp": xx * 2 + cc}

    def ymod(v):
        return lax.rem(v + NY, NY)

    def zmod(v):
        return lax.rem(v + NZ, NZ)

    arrivals = [
        pltpu.make_async_copy(src, dst, l_sem.at[i])
        for i, (src, dst) in enumerate((
            (gate_in, gate_sh), (up_in, up_sh), (down_in, down_sh), (outer_in, outer_sh), (inner_in, inner_sh),
            (value_in, value_sh), (mixer_in, mixer_sh), (stream_in, stream), (gains_in, gains_raw), (taps_in, taps_raw),
        ))
    ]
    for copy in arrivals:
        copy.start()

    y_fwd, y_back = at(z, ymod(y + s), x, c), at(z, ymod(y - s), x, c)
    z_fwd, z_back = at(zmod(z + s), y, x, c), at(zmod(z - s), y, x, c)
    mate = at(z, y, x, 1 - c)
    peers = [at(z, y, lax.rem(x + d, NX), c) for d in (1, 2, 3)]
    barrier = pltpu.get_barrier_semaphore()
    for dev in [y_fwd, y_back, z_fwd, z_back, mate] + peers:
        pl.semaphore_signal(barrier, inc=1, device_id=dev, device_id_type=pl.DeviceIdType.MESH)
    for copy in arrivals[:7]:
        copy.wait()

    def rows24(ref):
        return jnp.concatenate([ref[...].astype(F32), jnp.zeros((PAD - OWN, ref.shape[1]), F32)], axis=0)

    here = pl.ds(pl.multiple_of(y * PAD, 8), PAD)
    wa[c, z, here, 0:HID] = rows24(gate_sh).astype(BF16)
    wb[c, z, here, 0:HID] = rows24(up_sh).astype(BF16)
    down = rows24(down_sh).astype(BF16)
    wa[c, z, here, HID:HID + 128] = down[:, 0:128]
    wb[c, z, here, HID:HID + 256] = down[:, 128:HID]
    mix = jnp.concatenate(
        [rows24(outer_sh), rows24(inner_sh), rows24(value_sh), rows24(mixer_sh), jnp.zeros((PAD, 640 - 4 * CH), F32)], axis=1
    ).astype(BF16)
    ma[c, z, here, :] = mix[:, 0:384]
    mb[c, z, here, :] = mix[:, 384:640]
    pl.semaphore_wait(barrier, 8)

    ys = [y] + [ymod(y - s * d) for d in range(1, 5)] + [ymod(y + s * d) for d in range(1, 4)]
    zs = [z] + [zmod(z - s * d) for d in range(1, 7)] + [zmod(z + s * d) for d in range(1, 6)]
    bufs = (wa, wb, ma, mb)

    def remote(which, src_zz, src_yy, index, dev):
        ref = bufs[which].at[c, src_zz, pl.ds(pl.multiple_of(src_yy * PAD, 8), PAD), :]
        return pltpu.make_async_remote_copy(
            src_ref=ref, dst_ref=ref, send_sem=g_send.at[which, index], recv_sem=g_recv.at[which, index],
            device_id=dev, device_id_type=pl.DeviceIdType.MESH,
        )

    started = []

    def push(which, jz, jy, to_jz, to_jy, dev):
        copy = remote(which, zs[jz], ys[jy], to_jz * NY + to_jy, dev)
        copy.start()
        started.append(copy)

    def take(which, jz, jy):
        remote(which, zs[jz], ys[jy], jz * NY + jy, y_fwd).wait_recv()

    y_hops = ((0, 4, y_fwd), (4, 3, y_back))
    z_hops = ((0, 6, z_fwd), (6, 5, z_back))

    def y_next(which, jz, jy):
        for off, hops, dev in y_hops:
            if jy == 0:
                push(which, jz, 0, jz, off + 1, dev)
            elif off < jy < off + hops:
                push(which, jz, jy, jz, jy + 1, dev)

    def z_next(which, jz, jy):
        for off, hops, dev in z_hops:
            if jz == 0:
                push(which, 0, jy, off + 1, jy, dev)
            elif off < jz < off + hops:
                push(which, jz, jy, jz + 1, jy, dev)

    def y_far(jy):
        return jy if jy <= 4 else jy - 4

    def z_far(jz):
        return jz if jz <= 6 else jz - 6

    mates = []

    def to_mate(which, sub, index):
        ref = bufs[which].at[c, zs[index], pl.ds(0, NY * PAD), :] if which % 2 == 0 else sub
        copy = pltpu.make_async_remote_copy(
            src_ref=ref, dst_ref=ref, send_sem=p_send.at[which, index], recv_sem=p_recv.at[which, index],
            device_id=mate, device_id_type=pl.DeviceIdType.MESH,
        )
        copy.start()
        mates.append((which, copy))

    y_order = [0, 1, 5, 2, 6, 3, 7, 4]
    z_order = [0, 1, 7, 2, 8, 3, 9, 4, 10, 5, 11, 6]

    def own_out(group):
        even, odd = 2 * group, 2 * group + 1
        z_next(even, 0, 0)
        y_next(odd, 0, 0)
        y_next(even, 0, 0)
        z_next(odd, 0, 0)

    def slot_of(group, slot):
        even, odd = 2 * group, 2 * group + 1
        first = [(0, jy) for jy in y_order[1:]] + [(jz, jy) for jz in z_order[1:] for jy in y_order]
        second = [(jz, 0) for jz in z_order[1:]] + [(jz, jy) for jy in y_order[1:] for jz in z_order]
        first, second = (
            [(jz, jy) for jz, jy in blocks if z_far(jz) + y_far(jy) == slot] for blocks in (first, second)
        )
        for i in range(max(len(first), len(second))):
            for which, blocks in ((even, first), (odd, second)):
                if i < len(blocks):
                    jz, jy = blocks[i]
                    take(which, jz, jy)
                    if which == even or jy == 0:
                        z_next(which, jz, jy)
                    if which == odd or jz == 0:
                        y_next(which, jz, jy)
        for jz in range(NZ):
            if slot == 4 + z_far(jz):
                to_mate(even, None, jz)
        for jy in range(NY):
            if slot == 6 + y_far(jy):
                to_mate(odd, bufs[odd].at[c, :, pl.ds(pl.multiple_of(ys[jy] * PAD, 8), PAD), :], jy)

    def complete(group):
        for which, copy in mates:
            if which // 2 == group:
                copy.wait_recv()

    def token_rows(g, core, part_of, size):
        return pl.ds(pl.multiple_of((2 * g + core) * ROWS + part_of * SHARE, SHARE), size)

    def window(j, base, width):
        m = spread(j, base, width)
        to = slice(384 * j, 384 * (j + 1))
        everyone = lax.dot_general(
            stream[base:base + width, :], m, (((0,), (0,)), ((), ())), preferred_element_type=F32
        )
        fin[:, to] = everyone.astype(BF16)
        for g in range(GROUPS):
            xs[g * ROWS:(g + 1) * ROWS, to] = fin[token_rows(g, c, 0, ROWS), to]
            res[g, :, to] = fin[token_rows(g, c, x, SHARE), to]
        left = gains_raw[:, base:base + width]
        total = None
        for _ in range(3):
            term = left.astype(BF16)
            left = left - term.astype(F32)
            moved = dot(term, m)
            total = moved if total is None else total + moved
        gains[0:6, to] = total

    def first_norm():
        wide = xs[...].astype(F32)
        scale = lax.rsqrt(jnp.sum(wide * wide, axis=-1, keepdims=True) / D + EPSILON)
        for q in range(QN):
            cols = slice(q * QW, (q + 1) * QW)
            xn[q] = (wide[:, cols] * scale * gains[0:1, cols]).astype(BF16)

    def own_taps():
        for w in range(2):
            row = lax.broadcasted_iota(jnp.int32, (8 * CH, 256), 0)
            col = lax.broadcasted_iota(jnp.int32, (8 * CH, 256), 1)
            pick = jnp.where((row == col + (2 * x + w) * CH) & (col < CH), 1.0, 0.0).astype(BF16)
            taps[w, 0:3, :] = dot(taps_raw[...], pick)

    own_out(0)
    for copy in arrivals[7:]:
        copy.wait()
    for slot in range(1, 11):
        slot_of(0, slot)
        if slot > LAG:
            slot_of(1, slot - LAG)
        if slot == LAG:
            own_out(1)
        if slot <= 6:
            window(*windows()[slot - 1])
        if slot == 7:
            first_norm()
        if slot == 8:
            own_taps()
    later = list(range(11 - LAG, 11))
    complete(0)

    def weights(q, pieces):
        return jnp.concatenate(
            [buf[w, 4 * q:4 * q + 4, 0:NY * PAD, lo:hi].reshape(QW, hi - lo) for buf, w, lo, hi in pieces], axis=1
        )

    def mine(g, who):
        return pl.ds(pl.multiple_of(g * ROWS + who * SHARE, SHARE), SHARE)

    incoming, reduced = {}, {}

    def project(layer, g, terms):
        rows = slice(g * ROWS, (g + 1) * ROWS)
        for q in range(QN):
            for copy in incoming.get((layer, g, q), ()):
                copy.wait()
            for i, (buf, hi) in enumerate(terms):
                value = dot(xn[q, rows, :], weights(q, [(buf, w, 0, hi) for w in range(2)]))
                if q == 0:
                    proj[g, i, :, 0:2 * hi] = value
                else:
                    proj[g, i, :, 0:2 * hi] += value

    def scatter(layer, g, parts):
        for q in range(QN):
            part[layer, q, g * ROWS:(g + 1) * ROWS, :] = parts(q).astype(BF16)
            for d in (2, 1, 3):
                copy = pltpu.make_async_remote_copy(
                    src_ref=part.at[layer, q, mine(g, lax.rem(x + d, NX)), :],
                    dst_ref=got.at[g, d - 1, q],
                    send_sem=rs_send.at[layer, g, d - 1, q], recv_sem=rs_recv.at[layer, g, d - 1, q],
                    device_id=peers[d - 1], device_id_type=pl.DeviceIdType.MESH,
                )
                copy.start()
                reduced.setdefault((layer, g, q), []).append(copy)

    def settle(layer, g, gain, factor):
        squares = jnp.zeros((SHARE, 1), F32)
        for q in range(QN):
            for copy in reduced[layer, g, q]:
                copy.wait_recv()
            total = part[layer, q, mine(g, x), :].astype(F32)
            for d in range(3):
                total = total + got[g, d, q].astype(F32)
            tot[:, q * QW:(q + 1) * QW] = total
            squares = squares + jnp.sum(total * total, axis=-1, keepdims=True)
        scale = lax.rsqrt(squares / D + EPSILON)
        fresh = (res[g].astype(F32) + factor * (tot[...] * scale * gains[gain:gain + 1, :])).astype(BF16)
        res[g] = fresh
        return fresh

    def spread_rows(layer, g, gain, fresh):
        wide = fresh.astype(F32)
        scale = lax.rsqrt(jnp.sum(wide * wide, axis=-1, keepdims=True) / D + EPSILON)
        rows = mine(g, x)
        for q in range(QN):
            cols = slice(q * QW, (q + 1) * QW)
            xn[q, rows, :] = (wide[:, cols] * scale * gains[gain:gain + 1, cols]).astype(BF16)
            for d in (2, 1, 3):
                copy = pltpu.make_async_remote_copy(
                    src_ref=xn.at[q, rows, :], dst_ref=xn.at[q, rows, :],
                    send_sem=ag_send.at[layer, g, d - 1, q], recv_sem=ag_recv.at[layer, g, d - 1, q],
                    device_id=peers[d - 1], device_id_type=pl.DeviceIdType.MESH,
                )
                copy.start()
                incoming.setdefault((layer + 1, g, q), []).append(copy)

    def ffn(layer, g):
        project(layer, g, ((wa, HID), (wb, HID)))
        rows = slice(g * ROWS, (g + 1) * ROWS)
        gate, up = proj[g, 0], proj[g, 1]
        hid[rows, :] = (gate / (1.0 + jnp.exp(-gate)) * up).astype(BF16)

        def parts(q):
            down = [piece for w in range(2) for piece in ((wa, w, HID, HID + 128), (wb, w, HID, HID + 256))]
            return dot_t(hid[rows, :], weights(q, down))

        scatter(layer, g, parts)

    halos = []

    def mixer(g):
        project(1, g, ((ma, 384), (mb, 128)))
        gated, outer = [], []
        for w in range(2):
            both = jnp.concatenate(
                [proj[g, 0, :, w * 384:(w + 1) * 384], proj[g, 1, :, w * 128:(w + 1) * 128]], axis=1
            ).astype(BF16).astype(F32)
            outer.append(both[:, 0:CH])
            product = both[:, CH:2 * CH] * both[:, 2 * CH:3 * CH]
            gated.append(product)
            halo_out[g, w, :, 0:CH] = product[ROWS - 8:ROWS, :]
        copy = pltpu.make_async_remote_copy(
            src_ref=halo_out.at[g], dst_ref=halo_in.at[g], send_sem=h_send.at[g], recv_sem=h_recv.at[g],
            device_id=mate, device_id_type=pl.DeviceIdType.MESH,
        )
        copy.start()
        copy.wait()
        row = lax.broadcasted_iota(jnp.int32, (ROWS, CH), 0)
        for w in range(2):
            other = jnp.zeros((8, CH), F32) if g == 0 else halo_in[g - 1, w, :, 0:CH]
            before = jnp.where(c == 1, halo_in[g, w, :, 0:CH], other)
            one, two = before[7:8, :], before[6:7, :]
            now = gated[w]
            back1 = jnp.where(row == 0, one, pltpu.roll(now, 1, 0))
            back2 = pltpu.roll(now, 2, 0)
            back2 = jnp.where(row == 0, two, jnp.where(row == 1, one, back2))
            conv = taps[w, 0:1, 0:CH] * back2 + taps[w, 1:2, 0:CH] * back1 + taps[w, 2:3, 0:CH] * now
            mixed = outer[w] * conv
            hid[g * ROWS:(g + 1) * ROWS, w * 256:(w + 1) * 256] = jnp.concatenate(
                [jnp.zeros((ROWS, 12), F32), mixed, jnp.zeros((ROWS, 112), F32)], axis=1
            ).astype(BF16)
        rows = slice(g * ROWS, (g + 1) * ROWS)
        scatter(1, g, lambda q: dot_t(hid[rows, 0:512], weights(q, [(mb, 0, 0, 256), (mb, 1, 0, 256)])))

    def mixer_weights(count):
        for _ in range(count):
            if later:
                slot_of(1, later.pop(0))

    ffn(0, 0)
    mixer_weights(1)
    ffn(0, 1)
    mixer_weights(1)
    spread_rows(0, 0, 2, settle(0, 0, 1, 0.5))
    mixer_weights(1)
    spread_rows(0, 1, 2, settle(0, 1, 1, 0.5))
    mixer_weights(10)
    complete(1)
    mixer(0)
    mixer(1)
    spread_rows(1, 0, 4, settle(1, 0, 3, 1.0))
    spread_rows(1, 1, 4, settle(1, 1, 3, 1.0))
    ffn(2, 0)
    ffn(2, 1)

    outs, mate_outs, backs = [], [], []

    def result(g, d, dev, sems):
        rows = token_rows(g, c, lax.rem(x + NX - d, NX), SHARE)
        return pltpu.make_async_remote_copy(
            src_ref=fin.at[rows, :], dst_ref=fin.at[rows, :], send_sem=sems[0].at[g, d], recv_sem=sems[1].at[g, d],
            device_id=dev, device_id_type=pl.DeviceIdType.MESH,
        )

    for g in range(GROUPS):
        fin[token_rows(g, c, x, SHARE), :] = settle(2, g, 5, 0.5)
        for d in (2, 1, 3):
            outs.append(pltpu.make_async_remote_copy(
                src_ref=fin.at[token_rows(g, c, x, SHARE), :], dst_ref=fin.at[token_rows(g, c, x, SHARE), :],
                send_sem=fo_send.at[g, d], recv_sem=fo_recv.at[g, d],
                device_id=peers[d - 1], device_id_type=pl.DeviceIdType.MESH,
            ))
            outs[-1].start()
        mate_outs.append(result(g, 0, mate, (fp_send, fp_recv)))
        mate_outs[-1].start()
    for g in range(GROUPS):
        for d in (1, 3, 2):
            result(g, d, mate, (fo_send, fo_recv)).wait_recv()
            mate_outs.append(result(g, d, mate, (fp_send, fp_recv)))
            mate_outs[-1].start()
        for d in range(NX):
            result(g, d, mate, (fp_send, fp_recv)).wait_recv()
        acc[...] = jnp.zeros_like(acc)
        for j, base, width in windows():
            acc[base:base + width, :] += dot_t(spread(j, base, width), fin[g * HALF:(g + 1) * HALF, 384 * j:384 * (j + 1)])
        fout[g] = acc[...].astype(BF16)
        backs.append(pltpu.make_async_copy(fout.at[g], out.at[:, pl.ds(g * HALF, HALF)], l_sem.at[g]))
        backs[-1].start()
    for copies in reduced.values():
        for copy in copies:
            copy.wait_send()
    for copy in started + [copy for _, copy in mates] + outs + mate_outs:
        copy.wait_send()
    for copy in backs:
        copy.wait()


def local(stream_in, norm_gains, gate_proj, up_proj, down_proj, outer_gate, inner_gate, value_proj, mixer_out, conv_taps):
    hbm = pl.BlockSpec(memory_space=pl.ANY)
    dma = pltpu.SemaphoreType.DMA
    return pl.pallas_call(
        kernel,
        out_shape=jax.ShapeDtypeStruct((D, 2 * HALF), BF16),
        in_specs=[hbm] * 10,
        out_specs=hbm,
        scratch_shapes=[
            pltpu.VMEM((OWN, HID), BF16), pltpu.VMEM((OWN, HID), BF16), pltpu.VMEM((OWN, HID), BF16),
            pltpu.VMEM((OWN, CH), BF16), pltpu.VMEM((OWN, CH), BF16), pltpu.VMEM((OWN, CH), BF16), pltpu.VMEM((OWN, CH), BF16),
            pltpu.VMEM((D, 2 * HALF), BF16), pltpu.VMEM((6, D), F32), pltpu.VMEM((3, 8 * CH), BF16),
            pltpu.VMEM((2, NZ, NY * PAD + 8, 512), BF16),
            pltpu.VMEM((2, NZ, NY * PAD + 8, 640), BF16),
            pltpu.VMEM((2, NZ, NY * PAD + 8, 384), BF16),
            pltpu.VMEM((2, NZ, NY * PAD + 8, 256), BF16),
            pltpu.VMEM((HALF, DP), BF16),
            pltpu.VMEM((QN, HALF, QW), BF16),
            pltpu.VMEM((GROUPS, 2, ROWS, 2 * HID), F32),
            pltpu.VMEM((HALF, 2 * HID), BF16),
            pltpu.VMEM((3, QN, HALF, QW), BF16),
            pltpu.VMEM((GROUPS, 3, QN, SHARE, QW), BF16),
            pltpu.VMEM((SHARE, DP), F32),
            pltpu.VMEM((GROUPS, SHARE, DP), BF16),
            pltpu.VMEM((2 * HALF, DP), BF16),
            pltpu.VMEM((D, HALF), F32),
            pltpu.VMEM((2, D, HALF), BF16),
            pltpu.VMEM((8, DP), F32),
            pltpu.VMEM((2, 8, 256), F32),
            pltpu.VMEM((GROUPS, 2, 8, 256), F32),
            pltpu.VMEM((GROUPS, 2, 8, 256), F32),
            dma((4, 96)), dma((4, 96)),
            dma((4, 12)), dma((4, 12)),
            dma((3, GROUPS, 3, 3)), dma((3, GROUPS, 3, 3)),
            dma((2, GROUPS, 3, 3)), dma((2, GROUPS, 3, 3)),
            dma((GROUPS, NX)), dma((GROUPS, NX)),
            dma((GROUPS, NX)), dma((GROUPS, NX)),
            dma((GROUPS,)), dma((GROUPS,)),
            dma((10,)),
        ],
        compiler_params=pltpu.CompilerParams(
            collective_id=0, has_side_effects=True, vmem_limit_bytes=58 * 1024 * 1024
        ),
        name="layer",
    )(gate_proj, up_proj, down_proj, outer_gate, inner_gate, value_proj, mixer_out, stream_in.T, norm_gains, conv_taps).T


def solution(mesh):
    return jax.shard_map(
        local,
        mesh=mesh,
        in_specs=(
            P("fs", None), P(), P("fs", "tp"), P("fs", "tp"), P("fs", "tp"),
            P("fs", "tp"), P("fs", "tp"), P("fs", "tp"), P("fs", "tp"), P(),
        ),
        out_specs=P("fs", None),
        check_vma=False,
    )
```

```python
import jax
import jax.numpy as jnp
from jax import lax
from jax.experimental import pallas as pl
from jax.experimental.pallas import tpu as pltpu
from jax.sharding import PartitionSpec as P

EPSILON = 1e-06
NX, NY, NZ = 4, 8, 12
D = 2112
OWN = 22
PAD = 24
DP = 96 * PAD
QN, QW = 3, DP // 3
GROUPS, HALF = 2, 128
ROWS, SHARE = HALF // GROUPS, 16
HID, CH = 384, 132
SLOTS = 8
FOLLOW = {2: (1,), 3: (2,), 7: (3,)}
F32, BF16 = jnp.float32, jnp.bfloat16


def windows():
    out = []
    for j in range(6):
        base = (352 * j) // 128 * 128
        out.append((j, base, min(512, D - base)))
    return out


def spread(j, base, width):
    row = lax.broadcasted_iota(jnp.int32, (width, 384), 0).astype(F32) + float(base)
    col = lax.broadcasted_iota(jnp.int32, (width, 384), 1).astype(F32)
    block = jnp.floor((col + 0.5) / float(PAD))
    inside = col - block * float(PAD)
    target = float(352 * j) + block * float(OWN) + inside
    hit = (row == target) & (inside < float(OWN) - 0.5)
    return jnp.where(hit, 1.0, 0.0).astype(BF16)


def dot(a, b):
    return lax.dot_general(a, b, (((1,), (0,)), ((), ())), preferred_element_type=F32)


def dot_t(a, b):
    return lax.dot_general(a, b, (((1,), (1,)), ((), ())), preferred_element_type=F32)


def kernel(
    gate_in, up_in, down_in, outer_in, inner_in, value_in, mixer_in, stream_in, gains_in, taps_in, out_a, out_b,
    gate_sh, up_sh, down_sh, outer_sh, inner_sh, value_sh, mixer_sh, stream, gains_raw, taps_raw,
    wa, wb, ma, mb, xs, xn, proj, hid, part, got, tot, res, fin, acc, fout, gains, taps, halo_out, halo_in,
    g_send, g_recv, p_send, p_recv, rs_send, rs_recv, ag_send, ag_recv,
    fo_send, fo_recv, fp_send, fp_recv, h_send, h_recv, l_sem,
):
    fs, tp = lax.axis_index("fs"), lax.axis_index("tp")
    z, y = fs // NY, fs % NY
    x, c = tp // 2, tp % 2
    s = 1 - 2 * c

    def at(zz, yy, xx, cc):
        return {"fs": zz * NY + yy, "tp": xx * 2 + cc}

    def ymod(v):
        return lax.rem(v + 2 * NY, NY)

    def zmod(v):
        return lax.rem(v + 2 * NZ, NZ)

    arrivals = [
        pltpu.make_async_copy(src, dst, l_sem.at[i])
        for i, (src, dst) in enumerate((
            (gate_in, gate_sh), (up_in, up_sh), (down_in, down_sh), (outer_in, outer_sh), (inner_in, inner_sh),
            (value_in, value_sh), (mixer_in, mixer_sh), (stream_in, stream), (gains_in, gains_raw), (taps_in, taps_raw),
        ))
    ]
    for copy in arrivals:
        copy.start()

    y_fwd, y_back = at(z, ymod(y + s), x, c), at(z, ymod(y - s), x, c)
    z_fwd, z_back = at(zmod(z + s), y, x, c), at(zmod(z - s), y, x, c)
    y_fwd2, y_back2 = at(z, ymod(y + 2 * s), x, c), at(z, ymod(y - 2 * s), x, c)
    z_fwd2, z_back2 = at(zmod(z + 2 * s), y, x, c), at(zmod(z - 2 * s), y, x, c)
    mate = at(z, y, x, 1 - c)
    peers = [at(z, y, lax.rem(x + d, NX), c) for d in (1, 2, 3)]
    barrier = pltpu.get_barrier_semaphore()
    for dev in [y_fwd, y_back, z_fwd, z_back, y_fwd2, y_back2, z_fwd2, z_back2, mate] + peers:
        pl.semaphore_signal(barrier, inc=1, device_id=dev, device_id_type=pl.DeviceIdType.MESH)
    for copy in arrivals[:7]:
        copy.wait()

    def rows24(ref):
        return jnp.concatenate([ref[...].astype(F32), jnp.zeros((PAD - OWN, ref.shape[1]), F32)], axis=0)

    here = pl.ds(pl.multiple_of(y * PAD, 8), PAD)
    wa[c, z, here, 0:HID] = rows24(gate_sh).astype(BF16)
    wb[c, z, here, 0:HID] = rows24(up_sh).astype(BF16)
    down = rows24(down_sh).astype(BF16)
    wa[c, z, here, HID:HID + 128] = down[:, 0:128]
    wb[c, z, here, HID:HID + 256] = down[:, 128:HID]
    mix = jnp.concatenate(
        [rows24(outer_sh), rows24(inner_sh), rows24(value_sh), rows24(mixer_sh), jnp.zeros((PAD, 640 - 4 * CH), F32)], axis=1
    ).astype(BF16)
    ma[c, z, here, :] = mix[:, 0:384]
    mb[c, z, here, :] = mix[:, 384:640]
    pl.semaphore_wait(barrier, 12)

    ys = [y] + [ymod(y - s * d) for d in range(1, 5)] + [ymod(y + s * d) for d in range(1, 4)]
    zs = [z] + [zmod(z - s * d) for d in range(1, 7)] + [zmod(z + s * d) for d in range(1, 6)]
    bufs = (wa, wb, ma, mb)

    def remote(which, src_zz, src_yy, index, dev):
        ref = bufs[which].at[c, src_zz, pl.ds(pl.multiple_of(src_yy * PAD, 8), PAD), :]
        return pltpu.make_async_remote_copy(
            src_ref=ref, dst_ref=ref, send_sem=g_send.at[which, index], recv_sem=g_recv.at[which, index],
            device_id=dev, device_id_type=pl.DeviceIdType.MESH,
        )

    started = []

    def push(which, jz, jy, to_jz, to_jy, dev):
        copy = remote(which, zs[jz], ys[jy], to_jz * NY + to_jy, dev)
        copy.start()
        started.append(copy)

    def take(which, jz, jy):
        remote(which, zs[jz], ys[jy], jz * NY + jy, y_fwd).wait_recv()

    y_hops = ((0, 4, y_fwd, y_fwd2), (4, 3, y_back, y_back2))
    z_hops = ((0, 6, z_fwd, z_fwd2), (6, 5, z_back, z_back2))

    def y_next(which, jz, jy):
        for off, hops, dev, _ in y_hops:
            if jy == 0:
                push(which, jz, 0, jz, off + 1, dev)
            elif off < jy < off + hops:
                push(which, jz, jy, jz, jy + 1, dev)

    def z_next(which, jz, jy):
        for off, hops, dev, _ in z_hops:
            if jz == 0:
                push(which, 0, jy, off + 1, jy, dev)
            elif off < jz < off + hops:
                push(which, jz, jy, jz + 1, jy, dev)

    def leap(which, jz, jy):
        along_z = which % 2 == 1
        own = jz if along_z else jy
        for off, hops, dev, dev2 in z_hops if along_z else y_hops:
            if own == 0:
                targets = ((off + 1, dev), (off + 2, dev2))
            elif off < own <= off + hops - 2:
                targets = ((own + 2, dev2),)
            else:
                targets = ()
            for to, where in targets:
                if along_z:
                    push(which, jz, 0, to, 0, where)
                else:
                    push(which, 0, jy, 0, to, where)

    def y_far(jy):
        return jy if jy <= 4 else jy - 4

    def z_far(jz):
        return jz if jz <= 6 else jz - 6

    mates = []

    def to_mate(which, sub, index):
        ref = bufs[which].at[c, zs[index], pl.ds(0, NY * PAD), :] if which % 2 == 0 else sub
        copy = pltpu.make_async_remote_copy(
            src_ref=ref, dst_ref=ref, send_sem=p_send.at[which, index], recv_sem=p_recv.at[which, index],
            device_id=mate, device_id_type=pl.DeviceIdType.MESH,
        )
        copy.start()
        mates.append((which, copy))

    y_order = [0, 1, 5, 2, 6, 3, 7, 4]
    z_order = [0, 1, 7, 2, 8, 3, 9, 4, 10, 5, 11, 6]

    def own_out(group):
        even, odd = 2 * group, 2 * group + 1
        leap(odd, 0, 0)
        leap(even, 0, 0)
        z_next(even, 0, 0)
        y_next(odd, 0, 0)

    def slot_of(group, slot):
        even, odd = 2 * group, 2 * group + 1
        first = [(0, jy) for jy in y_order[1:]] + [(jz, jy) for jz in z_order[1:] for jy in y_order]
        second = [(jz, 0) for jz in z_order[1:]] + [(jz, jy) for jy in y_order[1:] for jz in z_order]
        first = [(jz, jy) for jz, jy in first if z_far(jz) + (y_far(jy) + 1) // 2 == slot]
        second = [(jz, jy) for jz, jy in second if (z_far(jz) + 1) // 2 + y_far(jy) == slot]
        for i in range(max(len(first), len(second))):
            for which, blocks in ((even, first), (odd, second)):
                if i < len(blocks):
                    jz, jy = blocks[i]
                    take(which, jz, jy)
                    if (jz if which == even else jy) == 0:
                        leap(which, jz, jy)
                    if which == even:
                        z_next(which, jz, jy)
                    else:
                        y_next(which, jz, jy)
        for jz in range(NZ):
            if slot == 2 + z_far(jz):
                to_mate(even, None, jz)
        for jy in range(NY):
            if slot == 3 + y_far(jy):
                to_mate(odd, bufs[odd].at[c, :, pl.ds(pl.multiple_of(ys[jy] * PAD, 8), PAD), :], jy)

    def complete(group):
        for which, copy in mates:
            if which // 2 == group:
                copy.wait_recv()

    def token_rows(g, core, part_of, size):
        return pl.ds(pl.multiple_of((2 * g + core) * ROWS + part_of * SHARE, SHARE), size)

    def window(j, base, width):
        m = spread(j, base, width)
        to = slice(384 * j, 384 * (j + 1))
        everyone = lax.dot_general(
            stream[base:base + width, :], m, (((0,), (0,)), ((), ())), preferred_element_type=F32
        )
        fin[:, to] = everyone.astype(BF16)
        for g in range(GROUPS):
            xs[g * ROWS:(g + 1) * ROWS, to] = fin[token_rows(g, c, 0, ROWS), to]
            res[g, :, to] = fin[token_rows(g, c, x, SHARE), to]
        left = gains_raw[:, base:base + width]
        total = None
        for _ in range(3):
            term = left.astype(BF16)
            left = left - term.astype(F32)
            moved = dot(term, m)
            total = moved if total is None else total + moved
        gains[0:6, to] = total

    def first_norm():
        wide = xs[...].astype(F32)
        scale = lax.rsqrt(jnp.sum(wide * wide, axis=-1, keepdims=True) / D + EPSILON)
        for q in range(QN):
            cols = slice(q * QW, (q + 1) * QW)
            xn[q] = (wide[:, cols] * scale * gains[0:1, cols]).astype(BF16)

    def own_taps():
        for w in range(2):
            row = lax.broadcasted_iota(jnp.int32, (8 * CH, 256), 0)
            col = lax.broadcasted_iota(jnp.int32, (8 * CH, 256), 1)
            pick = jnp.where((row == col + (2 * x + w) * CH) & (col < CH), 1.0, 0.0).astype(BF16)
            taps[w, 0:3, :] = dot(taps_raw[...], pick)

    own_out(0)
    own_out(1)
    for copy in arrivals[7:]:
        copy.wait()
    for slot in range(1, SLOTS + 1):
        slot_of(0, slot)
        for follower in FOLLOW.get(slot, ()):
            slot_of(1, follower)
        if slot <= 6:
            window(*windows()[slot - 1])
        if slot == 7:
            first_norm()
        if slot == 8:
            own_taps()
    later = list(range(1 + max(slot for slots in FOLLOW.values() for slot in slots), SLOTS + 1))
    complete(0)

    def weights(q, pieces):
        return jnp.concatenate(
            [buf[w, 4 * q:4 * q + 4, 0:NY * PAD, lo:hi].reshape(QW, hi - lo) for buf, w, lo, hi in pieces], axis=1
        )

    def mine(g, who):
        return pl.ds(pl.multiple_of(g * ROWS + who * SHARE, SHARE), SHARE)

    incoming, reduced = {}, {}

    def project(layer, g, terms):
        rows = slice(g * ROWS, (g + 1) * ROWS)
        for q in range(QN):
            for copy in incoming.get((layer, g, q), ()):
                copy.wait()
            for i, (buf, hi) in enumerate(terms):
                value = dot(xn[q, rows, :], weights(q, [(buf, w, 0, hi) for w in range(2)]))
                if q == 0:
                    proj[g, i, :, 0:2 * hi] = value
                else:
                    proj[g, i, :, 0:2 * hi] += value

    def scatter(layer, g, parts):
        for q in range(QN):
            part[layer, q, g * ROWS:(g + 1) * ROWS, :] = parts(q).astype(BF16)
            for d in (2, 1, 3):
                copy = pltpu.make_async_remote_copy(
                    src_ref=part.at[layer, q, mine(g, lax.rem(x + d, NX)), :],
                    dst_ref=got.at[g, d - 1, q],
                    send_sem=rs_send.at[layer, g, d - 1, q], recv_sem=rs_recv.at[layer, g, d - 1, q],
                    device_id=peers[d - 1], device_id_type=pl.DeviceIdType.MESH,
                )
                copy.start()
                reduced.setdefault((layer, g, q), []).append(copy)

    def settle(layer, g, gain, factor):
        squares = jnp.zeros((SHARE, 1), F32)
        for q in range(QN):
            for copy in reduced[layer, g, q]:
                copy.wait_recv()
            total = part[layer, q, mine(g, x), :].astype(F32)
            for d in range(3):
                total = total + got[g, d, q].astype(F32)
            tot[:, q * QW:(q + 1) * QW] = total
            squares = squares + jnp.sum(total * total, axis=-1, keepdims=True)
        scale = lax.rsqrt(squares / D + EPSILON)
        fresh = (res[g].astype(F32) + factor * (tot[...] * scale * gains[gain:gain + 1, :])).astype(BF16)
        res[g] = fresh
        return fresh

    def spread_rows(layer, g, gain, fresh):
        wide = fresh.astype(F32)
        scale = lax.rsqrt(jnp.sum(wide * wide, axis=-1, keepdims=True) / D + EPSILON)
        rows = mine(g, x)
        for q in range(QN):
            cols = slice(q * QW, (q + 1) * QW)
            xn[q, rows, :] = (wide[:, cols] * scale * gains[gain:gain + 1, cols]).astype(BF16)
            for d in (2, 1, 3):
                copy = pltpu.make_async_remote_copy(
                    src_ref=xn.at[q, rows, :], dst_ref=xn.at[q, rows, :],
                    send_sem=ag_send.at[layer, g, d - 1, q], recv_sem=ag_recv.at[layer, g, d - 1, q],
                    device_id=peers[d - 1], device_id_type=pl.DeviceIdType.MESH,
                )
                copy.start()
                incoming.setdefault((layer + 1, g, q), []).append(copy)

    def ffn(layer, g):
        project(layer, g, ((wa, HID), (wb, HID)))
        rows = slice(g * ROWS, (g + 1) * ROWS)
        gate, up = proj[g, 0], proj[g, 1]
        hid[rows, :] = (gate / (1.0 + jnp.exp(-gate)) * up).astype(BF16)

        def parts(q):
            down = [piece for w in range(2) for piece in ((wa, w, HID, HID + 128), (wb, w, HID, HID + 256))]
            return dot_t(hid[rows, :], weights(q, down))

        scatter(layer, g, parts)

    halos = []

    def mixer(g):
        project(1, g, ((ma, 384), (mb, 128)))
        gated, outer = [], []
        for w in range(2):
            both = jnp.concatenate(
                [proj[g, 0, :, w * 384:(w + 1) * 384], proj[g, 1, :, w * 128:(w + 1) * 128]], axis=1
            ).astype(BF16).astype(F32)
            outer.append(both[:, 0:CH])
            product = both[:, CH:2 * CH] * both[:, 2 * CH:3 * CH]
            gated.append(product)
            halo_out[g, w, :, 0:CH] = product[ROWS - 8:ROWS, :]
        copy = pltpu.make_async_remote_copy(
            src_ref=halo_out.at[g], dst_ref=halo_in.at[g], send_sem=h_send.at[g], recv_sem=h_recv.at[g],
            device_id=mate, device_id_type=pl.DeviceIdType.MESH,
        )
        copy.start()
        copy.wait()
        row = lax.broadcasted_iota(jnp.int32, (ROWS, CH), 0)
        for w in range(2):
            other = jnp.zeros((8, CH), F32) if g == 0 else halo_in[g - 1, w, :, 0:CH]
            before = jnp.where(c == 1, halo_in[g, w, :, 0:CH], other)
            one, two = before[7:8, :], before[6:7, :]
            now = gated[w]
            back1 = jnp.where(row == 0, one, pltpu.roll(now, 1, 0))
            back2 = pltpu.roll(now, 2, 0)
            back2 = jnp.where(row == 0, two, jnp.where(row == 1, one, back2))
            conv = taps[w, 0:1, 0:CH] * back2 + taps[w, 1:2, 0:CH] * back1 + taps[w, 2:3, 0:CH] * now
            mixed = outer[w] * conv
            hid[g * ROWS:(g + 1) * ROWS, w * 256:(w + 1) * 256] = jnp.concatenate(
                [jnp.zeros((ROWS, 12), F32), mixed, jnp.zeros((ROWS, 112), F32)], axis=1
            ).astype(BF16)
        rows = slice(g * ROWS, (g + 1) * ROWS)
        scatter(1, g, lambda q: dot_t(hid[rows, 0:512], weights(q, [(mb, 0, 0, 256), (mb, 1, 0, 256)])))

    def mixer_weights(count):
        for _ in range(count):
            if later:
                slot_of(1, later.pop(0))

    ffn(0, 0)
    mixer_weights(1)
    ffn(0, 1)
    mixer_weights(1)
    spread_rows(0, 0, 2, settle(0, 0, 1, 0.5))
    mixer_weights(1)
    spread_rows(0, 1, 2, settle(0, 1, 1, 0.5))
    mixer_weights(10)
    complete(1)
    mixer(0)
    mixer(1)
    spread_rows(1, 0, 4, settle(1, 0, 3, 1.0))
    spread_rows(1, 1, 4, settle(1, 1, 3, 1.0))
    ffn(2, 0)
    ffn(2, 1)

    outs, mate_outs, backs = [], [], []

    def result(g, d, dev, sems):
        rows = token_rows(g, c, lax.rem(x + NX - d, NX), SHARE)
        return pltpu.make_async_remote_copy(
            src_ref=fin.at[rows, :], dst_ref=fin.at[rows, :], send_sem=sems[0].at[g, d], recv_sem=sems[1].at[g, d],
            device_id=dev, device_id_type=pl.DeviceIdType.MESH,
        )

    for g in range(GROUPS):
        fin[token_rows(g, c, x, SHARE), :] = settle(2, g, 5, 0.5)
        for d in (2, 1, 3):
            outs.append(pltpu.make_async_remote_copy(
                src_ref=fin.at[token_rows(g, c, x, SHARE), :], dst_ref=fin.at[token_rows(g, c, x, SHARE), :],
                send_sem=fo_send.at[g, d], recv_sem=fo_recv.at[g, d],
                device_id=peers[d - 1], device_id_type=pl.DeviceIdType.MESH,
            ))
            outs[-1].start()
        mate_outs.append(result(g, 0, mate, (fp_send, fp_recv)))
        mate_outs[-1].start()
    for g in range(GROUPS):
        for d in (1, 3, 2):
            result(g, d, mate, (fo_send, fo_recv)).wait_recv()
            mate_outs.append(result(g, d, mate, (fp_send, fp_recv)))
            mate_outs[-1].start()
        for d in range(NX):
            result(g, d, mate, (fp_send, fp_recv)).wait_recv()
        acc[...] = jnp.zeros_like(acc)
        for j, base, width in windows():
            acc[base:base + width, :] += dot_t(spread(j, base, width), fin[g * HALF:(g + 1) * HALF, 384 * j:384 * (j + 1)])
        fout[g] = acc[...].astype(BF16)
        backs.append(pltpu.make_async_copy(fout.at[g], (out_a, out_b)[g], l_sem.at[g]))
        backs[-1].start()
    for copies in reduced.values():
        for copy in copies:
            copy.wait_send()
    for copy in started + [copy for _, copy in mates] + outs + mate_outs:
        copy.wait_send()
    for copy in backs:
        copy.wait()


def local(stream_in, norm_gains, gate_proj, up_proj, down_proj, outer_gate, inner_gate, value_proj, mixer_out, conv_taps):
    hbm = pl.BlockSpec(memory_space=pl.ANY)
    dma = pltpu.SemaphoreType.DMA
    halves = pl.pallas_call(
        kernel,
        out_shape=[jax.ShapeDtypeStruct((D, HALF), BF16)] * GROUPS,
        in_specs=[hbm] * 10,
        out_specs=[hbm] * GROUPS,
        scratch_shapes=[
            pltpu.VMEM((OWN, HID), BF16), pltpu.VMEM((OWN, HID), BF16), pltpu.VMEM((OWN, HID), BF16),
            pltpu.VMEM((OWN, CH), BF16), pltpu.VMEM((OWN, CH), BF16), pltpu.VMEM((OWN, CH), BF16), pltpu.VMEM((OWN, CH), BF16),
            pltpu.VMEM((D, 2 * HALF), BF16), pltpu.VMEM((6, D), F32), pltpu.VMEM((3, 8 * CH), BF16),
            pltpu.VMEM((2, NZ, NY * PAD + 8, 512), BF16),
            pltpu.VMEM((2, NZ, NY * PAD + 8, 640), BF16),
            pltpu.VMEM((2, NZ, NY * PAD + 8, 384), BF16),
            pltpu.VMEM((2, NZ, NY * PAD + 8, 256), BF16),
            pltpu.VMEM((HALF, DP), BF16),
            pltpu.VMEM((QN, HALF, QW), BF16),
            pltpu.VMEM((GROUPS, 2, ROWS, 2 * HID), F32),
            pltpu.VMEM((HALF, 2 * HID), BF16),
            pltpu.VMEM((3, QN, HALF, QW), BF16),
            pltpu.VMEM((GROUPS, 3, QN, SHARE, QW), BF16),
            pltpu.VMEM((SHARE, DP), F32),
            pltpu.VMEM((GROUPS, SHARE, DP), BF16),
            pltpu.VMEM((2 * HALF, DP), BF16),
            pltpu.VMEM((D, HALF), F32),
            pltpu.VMEM((2, D, HALF), BF16),
            pltpu.VMEM((8, DP), F32),
            pltpu.VMEM((2, 8, 256), F32),
            pltpu.VMEM((GROUPS, 2, 8, 256), F32),
            pltpu.VMEM((GROUPS, 2, 8, 256), F32),
            dma((4, 96)), dma((4, 96)),
            dma((4, 12)), dma((4, 12)),
            dma((3, GROUPS, 3, 3)), dma((3, GROUPS, 3, 3)),
            dma((2, GROUPS, 3, 3)), dma((2, GROUPS, 3, 3)),
            dma((GROUPS, NX)), dma((GROUPS, NX)),
            dma((GROUPS, NX)), dma((GROUPS, NX)),
            dma((GROUPS,)), dma((GROUPS,)),
            dma((10,)),
        ],
        compiler_params=pltpu.CompilerParams(
            collective_id=0, has_side_effects=True, vmem_limit_bytes=58 * 1024 * 1024
        ),
        name="layer",
    )(gate_proj, up_proj, down_proj, outer_gate, inner_gate, value_proj, mixer_out, stream_in.T, norm_gains, conv_taps)
    return jnp.concatenate(halves, axis=1).T


def solution(mesh):
    return jax.shard_map(
        local,
        mesh=mesh,
        in_specs=(
            P("fs", None), P(), P("fs", "tp"), P("fs", "tp"), P("fs", "tp"),
            P("fs", "tp"), P("fs", "tp"), P("fs", "tp"), P("fs", "tp"), P(),
        ),
        out_specs=P("fs", None),
        check_vma=False,
    )
```
